768 devices in a mesh: rep: 3 (over z_hi), fs: 32 (over z_lo, y), tp: 8 (over x, core).
Axes of the slice: x: 4, y: 8, z: 12 (z_hi: 3, z_lo: 4; z = z_hi * 4 + z_lo), core: 2. Of those that a mesh axis runs over, the one named last changes fastest.
Arguments:
- gate_pre: bfloat16 [98304, 3072], P(('rep', 'fs'), 'tp'), may hold values from -6 to 6
- up_pre: bfloat16 [98304, 3072], P(('rep', 'fs'), 'tp'), may hold values from -6 to 6
- out_grad: bfloat16 [98304, 2048], P(('rep', 'fs')), may hold values from -8 to 8
- w_down: bfloat16 [3072, 2048], P('tp', 'fs'), may hold values from -0.109375 to 0.109375
Outputs:
- d_gate: bfloat16 [98304, 3072], P(('rep', 'fs'), 'tp')
- d_up: bfloat16 [98304, 3072], P(('rep', 'fs'), 'tp')
- grad_down: float32 [3072, 2048], P('tp', 'fs')
- row_energy: float32 [3072], P('tp')
The draws below stay inside these ranges and needn't reach their ends.
All inputs are finite; a program needn't handle non-finite values.
Results may differ from the reference program's by a relative error of at most 0.0034.
Values may be sent and summed in bfloat16 or wider, within the bound.
No kernel may reach another device: no remote copies, remote signals or barrier semaphores. Data moves between devices by JAX's collectives and lax.ppermute only.
A program may use at most 32 MiB of HBM per device.

```python
import jax
import jax.numpy as jnp
from jax import lax

D = 2048
FF = 3072
TOK_DEV = 1024
TOKENS = 98304


def level_of(key, extent, split, low, high):
    loudness = 1.0
    for dim, shards_of in split:
        steps = jax.random.uniform(jax.random.fold_in(jax.random.fold_in(key, 6), dim), (shards_of,), jnp.float32, low / len(split), high / len(split))
        loudness = loudness * jnp.repeat(jnp.exp(steps), extent[dim] // shards_of).reshape((-1,) + (1,) * (len(extent) - 1 - dim))
    return loudness


def centred(stream_key, extent, width, limit, split=(), kind=jnp.bfloat16):
    entries = width * jax.random.normal(stream_key, extent, jnp.float32)
    if split:
        entries = entries * level_of(stream_key, extent, split, -0.22, 0.18)
    return jnp.clip(entries, -limit, limit).astype(kind)


def setup_inputs(seed: int = 0) -> dict:
    key_of = jax.random.split(jax.random.key(seed), 5)
    return {
        "gate_pre": centred(key_of[0], (TOKENS, FF), 1.0, 6.0, ((0, 96), (1, 8))),
        "up_pre": centred(key_of[1], (TOKENS, FF), 1.0, 6.0, ((0, 96), (1, 8))),
        "out_grad": centred(key_of[2], (TOKENS, D), 1.0, 8.0, ((0, 96),)),
        "w_down": centred(key_of[3], (FF, D), FF ** -0.5, 0.109375, ((0, 8), (1, 32))),
    }


def reference(gate_pre, up_pre, out_grad, w_down):
    blocks = TOKENS // TOK_DEV
    gate_blocks = gate_pre.reshape(blocks, TOK_DEV, FF)
    up_blocks = up_pre.reshape(blocks, TOK_DEV, FF)
    grad_blocks = out_grad.reshape(blocks, TOK_DEV, D)

    def step(total, items):
        gate_rows, up_rows, cot_rows = items
        gate_f = gate_rows.astype(jnp.float32)
        up_f = up_rows.astype(jnp.float32)
        sig = jax.nn.sigmoid(gate_f)
        act = gate_f * sig
        hidden = (act * up_f).astype(jnp.bfloat16)
        dhid = jnp.dot(cot_rows, w_down.T, preferred_element_type=jnp.float32)
        d_up = (dhid * act).astype(jnp.bfloat16)
        d_gate = (dhid * up_f * sig * (1.0 + gate_f * (1.0 - sig))).astype(jnp.bfloat16)
        total = total + jnp.dot(hidden.T, cot_rows, preferred_element_type=jnp.float32)
        return total, (d_gate, d_up)

    start = jnp.zeros((FF, D), jnp.float32)
    summed, outs = lax.scan(step, start, (gate_blocks, up_blocks, grad_blocks))
    grad_down = summed * (float(TOKENS) ** -0.5)
    row_energy = jnp.sum(grad_down * grad_down, axis=1) / D
    d_gate = outs[0].reshape(TOKENS, FF)
    d_up = outs[1].reshape(TOKENS, FF)
    return d_gate, d_up, grad_down, row_energy
```

```python
import functools

import jax
import jax.numpy as jnp
from jax import lax
from jax.experimental import pallas as pl
from jax.experimental.pallas import tpu as pltpu
from jax.sharding import Mesh
from jax.sharding import PartitionSpec as P


D = 2048
FS = ("fs_0", "fs_1")
REP_FS = ("rep", "fs_0", "fs_1")
HOPS = (1, -1, 2)


def swap(blocks, axis):
    return lax.all_to_all(blocks, axis, 0, 0, tiled=True)


def moved(value, hops):
    reps, depth, tp = (lax.axis_size(a) for a in ("rep", "fs_0", "tp"))
    ring = reps * depth
    pairs = []
    for z in range(ring):
        for t in range(tp):
            by = -hops if abs(hops) == 2 and t % 2 else hops
            pairs.append((z * tp + t, (z + by) % ring * tp + t))
    return lax.ppermute(value, ("rep", "fs_0", "tp"), pairs)


def in_vmem(kernel, shapes, *values):
    spec = pl.BlockSpec(memory_space=pltpu.VMEM)
    return pl.pallas_call(
        kernel,
        in_specs=[spec] * len(values),
        out_specs=[spec] * len(shapes),
        out_shape=[pltpu.VMEM(shape, kind) for shape, kind in shapes],
    )(*(pltpu.with_memory_space_constraint(v, pltpu.VMEM) for v in values))


def partial_kernel(first_ref, gate_ref, up_ref, cot_ref, out1, out2, out3, own, hidden_ref):
    step = pl.program_id(0)

    @pl.when(step == 0)
    def _():
        gate = gate_ref[...].astype(jnp.float32)
        hidden = gate * jax.nn.sigmoid(gate) * up_ref[...].astype(jnp.float32)
        hidden_ref[...] = hidden.T.astype(jnp.bfloat16)

    for k, out in enumerate((out1, out2, out3, own)):

        @pl.when(step == k)
        def _(out=out):
            part = jnp.dot(hidden_ref[...], cot_ref[...], preferred_element_type=jnp.float32)
            out[...] = part.astype(out.dtype)


def partial_grad(first, gate, up, cot):
    tokens, units = gate.shape
    cols = cot.shape[1] // 4

    def block(i, first):
        hops = jnp.where(i == 0, HOPS[0], jnp.where(i == 1, HOPS[1], jnp.where(i == 2, HOPS[2], 0)))
        return (0, lax.rem(first[0] + hops + 4, 4))

    whole = lambda i, first: (0, 0)
    return pl.pallas_call(
        partial_kernel,
        grid_spec=pltpu.PrefetchScalarGridSpec(
            num_scalar_prefetch=1,
            grid=(4,),
            in_specs=[
                pl.BlockSpec((tokens, units), whole),
                pl.BlockSpec((tokens, units), whole),
                pl.BlockSpec((tokens, cols), block),
            ],
            out_specs=[pl.BlockSpec(memory_space=pltpu.VMEM)] * 4,
            scratch_shapes=[pltpu.VMEM((units, tokens), jnp.bfloat16)],
        ),
        out_shape=[pltpu.VMEM((units, cols), jnp.bfloat16)] * 3
        + [pltpu.VMEM((units, cols), jnp.float32)],
        compiler_params=pltpu.CompilerParams(dimension_semantics=("arbitrary",)),
        name="partial_grad",
    )(first, gate, up, cot)


def window_kernel(own_ref, got1, got2, got3, out_ref):
    total = own_ref[...]
    for got in (got1, got2, got3):
        total = total + got[...].astype(jnp.float32)
    out_ref[...] = total.T.reshape(out_ref.shape).astype(out_ref.dtype)


def sum_kernel(got_ref, out_ref):
    total = jnp.sum(got_ref[...].astype(jnp.float32), axis=0)
    out_ref[...] = jnp.broadcast_to(total.astype(out_ref.dtype)[None], out_ref.shape)


def finish_kernel(factor, got_ref, grad_ref, rows_ref):
    grad = jnp.sum(got_ref[...].astype(jnp.float32), axis=0) * factor
    grad_ref[...] = grad
    rows_ref[...] = jnp.broadcast_to(
        jnp.sum(grad * grad, axis=0, keepdims=True)[None], rows_ref.shape
    )


def input_kernel(first_ref, gate_ref, up_ref, cot_ref, w0, w1, w2, w3, dgate_ref, dup_ref):
    first = first_ref[0]
    rows = w0.shape[0]
    dhid = None
    for hops, w in zip((0, 1, -1, 2), (w0, w1, w2, w3)):
        at = pl.multiple_of(lax.rem(first - hops + 4, 4) * rows, rows)
        term = jnp.dot(cot_ref[:, pl.ds(at, rows)], w[...], preferred_element_type=jnp.float32)
        dhid = term if dhid is None else dhid + term
    gate = gate_ref[...].astype(jnp.float32)
    up = up_ref[...].astype(jnp.float32)
    sig = jax.nn.sigmoid(gate)
    dup_ref[...] = (dhid * (gate * sig)).astype(jnp.bfloat16)
    dgate_ref[...] = (dhid * up * sig * (1.0 + gate * (1.0 - sig))).astype(jnp.bfloat16)


def input_grads(first, gate, up, cot, weights, step=256):
    tokens, units = gate.shape
    width = cot.shape[1]
    rows = lambda i, first: (i, 0)
    return pl.pallas_call(
        input_kernel,
        grid_spec=pltpu.PrefetchScalarGridSpec(
            num_scalar_prefetch=1,
            grid=(tokens // step,),
            in_specs=[
                pl.BlockSpec((step, units), rows),
                pl.BlockSpec((step, units), rows),
                pl.BlockSpec((step, width), rows),
            ]
            + [pl.BlockSpec(memory_space=pltpu.VMEM)] * 4,
            out_specs=[pl.BlockSpec((step, units), rows)] * 2,
        ),
        out_shape=[jax.ShapeDtypeStruct((tokens, units), jnp.bfloat16)] * 2,
        compiler_params=pltpu.CompilerParams(dimension_semantics=("arbitrary",)),
        name="input_grads",
    )(first, gate, up, cot, *(pltpu.with_memory_space_constraint(w, pltpu.VMEM) for w in weights))


def local(gate_pre, up_pre, out_grad, w_down):
    peers, reps, high = (lax.axis_size(a) for a in (FS, "rep", "fs_1"))
    factor = float(out_grad.shape[0] * reps * peers) ** (-0.5)
    units, cols = w_down.shape
    kind = jnp.bfloat16
    first = lax.axis_index("fs_0").astype(jnp.int32)[None]

    copies = jnp.broadcast_to(w_down.T[None], (high, cols, units))
    mine = swap(copies, "fs_1").reshape(-1, units)
    *away, own = partial_grad(first, gate_pre, up_pre, out_grad)
    got = [moved(part, hops) for part, hops in zip(away, HOPS)]
    (part,) = in_vmem(window_kernel, [((high, cols, units), kind)], own, *got)
    got = swap(part, "fs_1")
    weights = [mine] + [moved(mine, hops) for hops in HOPS]
    (total,) = in_vmem(sum_kernel, [((reps, cols, units), kind)], got)
    got = swap(total, "rep")
    grad, rows = in_vmem(
        functools.partial(finish_kernel, factor),
        [((cols, units), jnp.float32), ((peers, 1, units), jnp.float32)],
        got,
    )
    energy = jnp.sum(swap(rows, FS), axis=(0, 1)) / D
    d_gate, d_up = input_grads(first, gate_pre, up_pre, out_grad, weights)
    return d_gate, d_up, grad.T, energy


def solution(mesh):
    torus = Mesh(
        mesh.devices.reshape(mesh.shape["rep"], 4, 8, mesh.shape["tp"]),
        ("rep", "fs_0", "fs_1", "tp"),
    )
    placed = (P(REP_FS, "tp"), P(REP_FS, "tp"), P(REP_FS, None), P("tp", FS))
    return jax.shard_map(
        local,
        mesh=torus,
        in_specs=placed,
        out_specs=(P(REP_FS, "tp"), P(REP_FS, "tp"), P("tp", FS), P("tp")),
        check_vma=False,
    )
```
